32 devices in a mesh: fs: 8 (over z, x), tp: 4 (over y, core).
Axes of the slice: x: 2, y: 2, z: 4, core: 2. Of those that a mesh axis runs over, the one named last changes fastest.
Arguments:
- tokens: bfloat16 [320, 4096], P('fs'), may hold values from -6 to 6
- routes: int32 [320, 2], P('fs'), may hold values from 0 to 3, all different within a row; in each aligned block of 40 rows (0 to 39, 40 to 79, ...) at most 30 rows name the same one
- route_logits: float32 [320, 2], P('fs'), may hold values from -6 to 6
- norm_gain: float32 [4096], P('fs'), may hold values from 0.1 to 1.9
- gate_weight: float32 [4, 4096, 8192], P(None, 'fs', 'tp'), may hold values from -0.09375 to 0.09375
- up_weight: float32 [4, 4096, 8192], P(None, 'fs', 'tp'), may hold values from -0.09375 to 0.09375
- down_weight: float32 [4, 4096, 8192], P(None, 'fs', 'tp'), may hold values from -0.0625 to 0.0625
Outputs:
- mixed: bfloat16 [320, 4096], P('fs', 'tp')
- gate_sampler: bfloat16 [4, 4096, 8192], P('tp', None, 'fs')
- up_sampler: bfloat16 [4, 4096, 8192], P('tp', None, 'fs')
- down_sampler: bfloat16 [4, 4096, 8192], P('tp', None, 'fs')
The draws below stay inside these ranges and needn't reach their ends.
Inputs may be any that keep to these rules, and one draw needn't show every extreme that they name: `routes`: the 2 experts of a token differ. Within the tokens of one index of fs (aligned blocks of 40 rows) no expert is named by more than 30 tokens.
All inputs are finite; a program needn't handle non-finite values.
Results may differ from the reference program's by a relative error of at most 0.01.
Values may be sent and summed in bfloat16 or wider, within the bound.
No kernel may reach another device: no remote copies, remote signals or barrier semaphores. Data moves between devices by JAX's collectives and lax.ppermute only.
A program may use at most 192 MiB of HBM per device.

```python
import math
import jax
import jax.numpy as jnp
import numpy as np
from jax import lax

D = 4096
FF = 8192
EXPERTS = 4
TOPK = 2
TOK_DEV = 40
CAP = 30
TOKENS = 320
N_TP = 4


def block_scale(own_key, extent, pieces, least, high):
    gain = 1.0
    for dim, parts in pieces:
        heights = jax.random.uniform(jax.random.fold_in(jax.random.fold_in(own_key, 6), dim), (parts,), jnp.float32, least / len(pieces), high / len(pieces))
        gain = gain * jnp.repeat(jnp.exp(heights), extent[dim] // parts).reshape((-1,) + (1,) * (len(extent) - 1 - dim))
    return gain


def assign_block(own_key, own, number, rows, number_of, top, limit, lean):
    order = jax.random.permutation(own_key, number_of)
    heavy_load, usual = portions_of(number_of, rows * top, limit, lean, True), portions_of(number_of, rows * top, limit, lean, False)
    places = jnp.arange(number_of)

    def named(sizes, offset_by):
        used = int((sizes > 0).sum())
        fixed = max(1, used // 4)
        moved = fixed + (places - fixed + offset_by * (used - fixed)) % max(1, number_of - fixed)
        return jnp.zeros((number_of,), jnp.int32).at[order[jnp.where(places < fixed, places, moved)]].set(jnp.asarray(sizes, jnp.int32))

    sizes = jnp.where(number % 4 == 0, named(heavy_load, number // 4), named(usual, number - number // 4 - 1))
    mixed = jax.random.permutation(jax.random.fold_in(own, 3), number_of)
    donor, sink = mixed[0:number_of // 2 * 2:2], mixed[1:number_of // 2 * 2:2]
    room = jnp.minimum(sizes[donor] - 1, limit - sizes[sink]) // 2
    room = jnp.where((donor == order[0]) | (sink == order[0]) | (sizes[sink] == 0), 0, jnp.maximum(room, 0))
    moved = jax.random.randint(jax.random.fold_in(own, 4), (number_of // 2,), 0, 1 << 20) % (room + 1)
    sizes = sizes.at[donor].add(-moved).at[sink].add(moved)
    labels = jnp.searchsorted(jnp.cumsum(sizes), jnp.arange(rows * top), side="right").astype(jnp.int32)
    grid = labels.reshape(top, rows).T
    grid = grid[jax.random.permutation(jax.random.fold_in(own, 1), rows)]
    offset_by = jax.random.randint(jax.random.fold_in(own, 2), (rows, 1), 0, top)
    return jnp.take_along_axis(grid, (jnp.arange(top)[None, :] + offset_by) % top, axis=1)


def portions_of(count, total, most, slope, full):
    loads = [(1 << 20) // math.isqrt(rank ** slope) + 1 for rank in range(1, count + 1)]
    largest = most if full else min(most, max(-(-total // count), total * loads[0] // sum(loads)))
    least = 1 if total - largest >= count - 1 else 0
    holding, spare = [largest] + [least] * (count - 1), total - largest - least * (count - 1)
    while spare > 0:
        free = [i for i in range(1, count) if holding[i] < largest] or [i for i in range(1, count) if holding[i] < most]
        mass, remaining = sum([loads[i] for i in free]), spare
        for i in free:
            extra = min(most - holding[i], max(1, remaining * loads[i] // mass), spare)
            holding[i] = holding[i] + extra
            spare = spare - extra
    return np.array(holding)


def centred(key, extent, scale, reach, cuts=(), held_as=jnp.bfloat16):
    drawn = jax.random.normal(key, extent, jnp.float32) * scale
    if len(cuts) > 0:
        drawn = block_scale(key, extent, cuts, -0.22, 0.18) * drawn
    return jnp.clip(drawn, min=-reach, max=reach).astype(held_as)


def setup_inputs(seed: int = 0) -> dict:
    arg_keys = jax.random.split(jax.random.key(seed), 8)
    tokens = centred(arg_keys[0], (TOKENS, D), 1.0, 6.0, ((0, 8),))
    routes_keys = jax.random.split(jax.random.fold_in(arg_keys[1], 1), TOKENS // TOK_DEV)
    routes_turns = jax.random.permutation(jax.random.fold_in(arg_keys[1], 3), TOKENS // TOK_DEV)
    routes = jax.vmap(lambda own, number: assign_block(jax.random.fold_in(arg_keys[1], 2), own, number, TOK_DEV, EXPERTS, TOPK, CAP, 2))(routes_keys, routes_turns).reshape((TOKENS, TOPK))
    route_logits = centred(arg_keys[2], (TOKENS, TOPK), 1.5, 6.0, ((0, 8),), jnp.float32)
    norm_gain = jnp.clip(1.0 + 0.18 * jax.random.normal(arg_keys[3], (D,), jnp.float32), 0.1, 1.9)
    gate_weight = centred(arg_keys[4], (EXPERTS, D, FF), D ** -0.5, 0.09375, ((1, 8), (2, 4)), jnp.float32)
    up_weight = centred(arg_keys[5], (EXPERTS, D, FF), D ** -0.5, 0.09375, ((1, 8), (2, 4)), jnp.float32)
    down_weight = centred(arg_keys[6], (EXPERTS, D, FF), FF ** -0.5, 0.0625, ((1, 8), (2, 4)), jnp.float32)
    return {"tokens": tokens, "routes": routes, "route_logits": route_logits, "norm_gain": norm_gain, "gate_weight": gate_weight, "up_weight": up_weight, "down_weight": down_weight}


def arrange(matrix):
    experts, width, hidden_units = matrix.shape
    block = hidden_units // N_TP
    split = matrix.reshape(experts, width, N_TP, block)
    return jnp.transpose(split, (2, 1, 0, 3)).reshape(N_TP, width, experts * block)

def reference(tokens, routes, route_logits, norm_gain, gate_weight, up_weight, down_weight):
    gain_cols = norm_gain.astype(jnp.float32)[None, :, None]
    folded_gate = (gate_weight * gain_cols).astype(jnp.bfloat16)
    folded_up = (up_weight * gain_cols).astype(jnp.bfloat16)
    rounded_down = down_weight.astype(jnp.bfloat16)
    tok_float = tokens.astype(jnp.float32)
    normed = (tok_float * lax.rsqrt(lax.optimization_barrier(jnp.mean(tok_float * tok_float, axis=1, keepdims=True)) + 1e-05)).astype(jnp.bfloat16)
    shares = jax.nn.sigmoid(route_logits - route_logits[:, ::-1])
    mixed = jnp.zeros((tokens.shape[0], tokens.shape[1]), jnp.float32)
    for expert in range(EXPERTS):
        gate_act = jnp.dot(normed, folded_gate[expert], preferred_element_type=jnp.float32)
        up_act = jnp.dot(normed, folded_up[expert], preferred_element_type=jnp.float32)
        hidden = (jax.nn.silu(gate_act) * up_act).astype(jnp.bfloat16)
        expert_out = lax.dot_general(hidden, rounded_down[expert], (((1,), (1,)), ((), ())), preferred_element_type=jnp.float32)
        weight = lax.optimization_barrier(jnp.sum(jnp.where(routes == expert, shares, 0.0), axis=1))
        mixed = mixed + weight[:, None] * expert_out
    return (mixed.astype(jnp.bfloat16), arrange(folded_gate), arrange(folded_up), arrange(rounded_down))
```

```python
import functools

import jax
import jax.numpy as jnp
from jax import lax
from jax.experimental import pallas as pl
from jax.experimental.pallas import tpu as pltpu
from jax.sharding import PartitionSpec as P


HBM = pltpu.MemorySpace.HBM
VMEM = pltpu.MemorySpace.VMEM
SMEM = pltpu.MemorySpace.SMEM


def swap(value, axis, k):
    count = lax.axis_size(axis)
    return lax.ppermute(value, axis, [(i, i ^ k) for i in range(count)])


def partner_order(count):
    far = list(range(count // 2, count))
    near = list(range(1, count // 2))
    order = []
    while far or near:
        if far:
            order.append(far.pop(0))
        if near:
            order.append(near.pop(0))
    return order


def fold_kernel(where_ref, weight_ref, gain_ref, out_ref):
    out_ref[...] = (weight_ref[0] * gain_ref[...]).astype(jnp.bfloat16)


def round_kernel(where_ref, weight_ref, out_ref):
    out_ref[...] = weight_ref[0].astype(jnp.bfloat16)


def make_piece(weight, gain, dest, spread, columns, start, rows):
    block = min(rows, 128)
    where = jnp.stack([dest // spread, dest % spread]).astype(jnp.int32)
    first = start // block
    in_specs = [pl.BlockSpec((1, block, columns), lambda i, w: (w[0], i + first, w[1]))]
    args = [weight]
    body = round_kernel
    if gain is not None:
        in_specs.append(pl.BlockSpec((block, 1), lambda i, w: (i + first, 0)))
        args.append(gain)
        body = fold_kernel
    return pl.pallas_call(
        body,
        grid_spec=pltpu.PrefetchScalarGridSpec(
            num_scalar_prefetch=1,
            grid=(rows // block,),
            in_specs=in_specs,
            out_specs=pl.BlockSpec((block, columns), lambda i, w: (i, 0)),
        ),
        out_shape=jax.ShapeDtypeStruct((rows, columns), jnp.bfloat16),
    )(where, *args)


def act_kernel(count, per_tp, keys, hidden, *refs):
    me_ref, x_ref = refs[:2]
    pieces = refs[2 : 2 + count]
    refs = refs[2 + count :]
    if hidden:
        gate_ref, out_ref, act_ref, held, acc, load_sem, store_sem = refs
    else:
        out_ref, act_ref, held, acc, load_sem, store_sem = refs
    rows = pieces[0].shape[0]
    loads = [
        pltpu.make_async_copy(pieces[j], held.at[j], load_sem.at[j]) for j in range(count)
    ]
    for load in loads:
        load.start()
    stores = []
    for j in range(count):
        slot = me_ref[0] ^ keys[j]
        loads[j].wait()
        store = pltpu.make_async_copy(
            held.at[j], out_ref.at[pl.ds(pl.multiple_of(slot * rows, rows), rows)], store_sem.at[j]
        )
        store.start()
        stores.append(store)
        which = (slot // per_tp ^ me_ref[1]) * per_tp + slot % per_tp
        part = jnp.dot(x_ref[which], held[j], preferred_element_type=jnp.float32)
        if j == 0:
            acc[...] = part
        else:
            acc[...] += part
    if hidden:
        gate = gate_ref[...]
        act_ref[...] = (gate / (1.0 + jnp.exp(-gate)) * acc[...]).astype(jnp.bfloat16)
    else:
        act_ref[...] = acc[...]
    for store in stores:
        store.wait()


def activate(me, x, pieces, keys, per_tp, gate=None):
    count = len(pieces)
    rows, columns = pieces[0].shape
    tokens = x.shape[1]
    args = [me, x, *pieces]
    in_specs = [pl.BlockSpec(memory_space=SMEM), pl.BlockSpec(memory_space=VMEM)]
    in_specs += [pl.BlockSpec(memory_space=HBM)] * count
    if gate is not None:
        args.append(gate)
        in_specs.append(pl.BlockSpec(memory_space=VMEM))
    act_type = jnp.float32 if gate is None else jnp.bfloat16
    return pl.pallas_call(
        functools.partial(act_kernel, count, per_tp, keys, gate is not None),
        in_specs=in_specs,
        out_specs=[pl.BlockSpec(memory_space=HBM), pl.BlockSpec(memory_space=VMEM)],
        out_shape=[
            jax.ShapeDtypeStruct((count * rows, columns), jnp.bfloat16),
            jax.ShapeDtypeStruct((tokens, columns), act_type),
        ],
        scratch_shapes=[
            pltpu.VMEM((count, rows, columns), jnp.bfloat16),
            pltpu.VMEM((tokens, columns), jnp.float32),
            pltpu.SemaphoreType.DMA((count,)),
            pltpu.SemaphoreType.DMA((count,)),
        ],
    )(*args)


def down_kernel(count, per_tp, keys, me_ref, hidden_ref, weight_ref, *refs):
    pieces = refs[:count]
    keep_ref, send_ref, held, sums, load_sem, store_sem = refs[count:]
    loads = [
        pltpu.make_async_copy(pieces[j], held.at[j], load_sem.at[j]) for j in range(count)
    ]
    for load in loads:
        load.start()
    for j in range(count):
        slot = me_ref[0] ^ keys[j]
        loads[j].wait()
        part = lax.dot_general(
            hidden_ref[...],
            held[j],
            (((1,), (1,)), ((), ())),
            preferred_element_type=jnp.float32,
        )
        block = slot // per_tp
        side = (block ^ me_ref[1]) & 1
        place = (side * (count // 2)) + (block // 2) * per_tp + slot % per_tp
        sums[place] = (part * weight_ref[...]).astype(jnp.bfloat16)
    half = count // 2
    keep = pltpu.make_async_copy(sums.at[pl.ds(0, half)], keep_ref, store_sem.at[0])
    send = pltpu.make_async_copy(sums.at[pl.ds(half, half)], send_ref, store_sem.at[1])
    send.start()
    keep.start()
    send.wait()
    keep.wait()


def down_partial(me, hidden, weight, pieces, keys, per_tp):
    count = len(pieces)
    rows, columns = pieces[0].shape
    tokens = hidden.shape[0]
    half = jax.ShapeDtypeStruct((count // 2, tokens, rows), jnp.bfloat16)
    return pl.pallas_call(
        functools.partial(down_kernel, count, per_tp, keys),
        in_specs=[
            pl.BlockSpec(memory_space=SMEM),
            pl.BlockSpec(memory_space=VMEM),
            pl.BlockSpec(memory_space=VMEM),
        ]
        + [pl.BlockSpec(memory_space=HBM)] * count,
        out_specs=[pl.BlockSpec(memory_space=HBM)] * 2,
        out_shape=[half, half],
        scratch_shapes=[
            pltpu.VMEM((count, rows, columns), jnp.bfloat16),
            pltpu.VMEM((count, tokens, rows), jnp.bfloat16),
            pltpu.SemaphoreType.DMA((count,)),
            pltpu.SemaphoreType.DMA((2,)),
        ],
    )(me, hidden, weight, *pieces)


def place_kernel(count, keys, width, start, aliased, me_ref, *refs):
    pieces = refs[:count]
    out_ref, sem = refs[-2:]
    rows = pieces[0].shape[0]
    copies = []
    for j in range(count):
        slot = me_ref[0] ^ keys[j]
        first = pl.multiple_of(slot * width + start, 16)
        copy = pltpu.make_async_copy(pieces[j], out_ref.at[pl.ds(first, rows)], sem.at[j])
        copy.start()
        copies.append(copy)
    for copy in copies:
        copy.wait()


def place_chunk(me, pieces, keys, width, start, out):
    count = len(pieces)
    columns = pieces[0].shape[1]
    args = [me, *pieces]
    in_specs = [pl.BlockSpec(memory_space=SMEM)] + [pl.BlockSpec(memory_space=HBM)] * count
    aliases = {}
    if out is not None:
        aliases = {len(args): 0}
        args.append(out)
        in_specs.append(pl.BlockSpec(memory_space=HBM))
    return pl.pallas_call(
        functools.partial(place_kernel, count, keys, width, start, out is not None),
        in_specs=in_specs,
        out_specs=pl.BlockSpec(memory_space=HBM),
        out_shape=jax.ShapeDtypeStruct((count * width, columns), jnp.bfloat16),
        scratch_shapes=[pltpu.SemaphoreType.DMA((count,))],
        input_output_aliases=aliases,
    )(*args)


def reduce_tp(keep, send, per_tp):
    tp_count = lax.axis_size("tp")
    me = lax.axis_index("tp")
    total = keep.astype(jnp.float32) + swap(send, "tp", 1).astype(jnp.float32)
    left = tp_count // 2
    total = total.reshape((left, per_tp) + keep.shape[1:])
    bit = 2
    while left > 1:
        split = total.reshape((left // 2, 2) + total.shape[1:])
        mine = (me // bit) % 2
        stay = lax.dynamic_index_in_dim(split, mine, 1, keepdims=False)
        go = lax.dynamic_index_in_dim(split, 1 - mine, 1, keepdims=False).astype(jnp.bfloat16)
        total = stay + swap(go, "tp", bit).astype(jnp.float32)
        left //= 2
        bit *= 2
    return total[0]


def per_device(tokens, routes, route_logits, norm_gain, gate_weight, up_weight, down_weight):
    experts, width, _ = gate_weight.shape
    fs_count, tp_count = lax.axis_size("fs"), lax.axis_size("tp")
    fs_me, tp_me = lax.axis_index("fs"), lax.axis_index("tp")
    spread = fs_count // experts
    per_tp = fs_count // tp_count
    columns = gate_weight.shape[2] // spread
    own_rows, model = tokens.shape
    me = jnp.stack([fs_me, tp_me]).astype(jnp.int32)
    gain = norm_gain[:, None]
    order = partner_order(fs_count)
    keys = [0] + order

    def exchange(weight, gain, start, rows):
        arrived = []
        for k in order:
            piece = make_piece(weight, gain, fs_me ^ k, spread, columns, start, rows)
            arrived.append(swap(piece, "fs", k))
        own = make_piece(weight, gain, fs_me, spread, columns, start, rows)
        return [own] + arrived

    gate_pieces = exchange(gate_weight, gain, 0, width)

    tok_float = tokens.astype(jnp.float32)
    normed = (
        tok_float * lax.rsqrt(jnp.mean(tok_float * tok_float, axis=1, keepdims=True) + 1e-05)
    ).astype(jnp.bfloat16)
    part_width = model // tp_count
    own_cols = lax.dynamic_slice_in_dim(normed, tp_me * part_width, part_width, 1)
    shares = jax.nn.sigmoid(route_logits - route_logits[:, ::-1])
    expert_ids = lax.broadcasted_iota(jnp.int32, (1, 1, experts), 2)
    weights = jnp.sum(jnp.where(routes[:, :, None] == expert_ids, shares[:, :, None], 0.0), axis=1)
    terms, rest = [], weights
    for _ in range(3):
        term = lax.reduce_precision(rest, 8, 7)
        terms.append(term.astype(jnp.bfloat16))
        rest = rest - term
    extra = jnp.concatenate(terms, axis=1)
    extra = jnp.pad(extra, ((0, 0), (0, -extra.shape[1] % 128)))
    packet = jnp.concatenate([own_cols, extra], axis=1)
    packet = jnp.broadcast_to(packet[None], (fs_count,) + packet.shape)
    gathered = lax.all_to_all(packet, "fs", split_axis=0, concat_axis=0, tiled=True)
    gathered = gathered.reshape(fs_count * own_rows, packet.shape[2])
    block = gathered[:, :part_width]
    term_cols = gathered[:, part_width : part_width + 3 * experts].astype(jnp.float32)
    row_weights = jnp.sum(term_cols.reshape(-1, 3, experts), axis=1)
    mine = lax.broadcasted_iota(jnp.int32, (1, experts), 1) == fs_me // spread
    row_weight = jnp.sum(jnp.where(mine, row_weights, 0.0), axis=1, keepdims=True)
    blocks = jnp.stack([block] + [swap(block, "tp", k) for k in range(1, tp_count)])
    x = blocks.reshape(tp_count, -1, per_tp, width)
    x = jnp.transpose(x, (0, 2, 1, 3)).reshape(fs_count, -1, width)

    up_pieces = exchange(up_weight, gain, 0, width)
    cuts = [0, width * 3 // 4, width]
    chunks = [
        exchange(down_weight, None, first, last - first) for first, last in zip(cuts, cuts[1:])
    ]

    gate_out, gate_act = activate(me, x, gate_pieces, keys, per_tp)
    up_out, hidden = activate(me, x, up_pieces, keys, per_tp, gate_act)

    down_out = None
    parts = []
    for start, pieces in zip(cuts, chunks):
        keep, send = down_partial(me, hidden, row_weight, pieces, keys, per_tp)
        total = reduce_tp(keep, send, per_tp)
        rows = total.shape[2]
        total = total.reshape(per_tp, fs_count, own_rows, rows)
        total = jnp.transpose(total, (1, 0, 2, 3)).astype(jnp.bfloat16)
        back = lax.all_to_all(total, "fs", split_axis=0, concat_axis=0, tiled=True)
        parts.append(jnp.sum(back.astype(jnp.float32), axis=0).astype(jnp.bfloat16))
        down_out = place_chunk(me, pieces, keys, width, start, down_out)
    mixed = jnp.concatenate(parts, axis=2)
    mixed = jnp.transpose(mixed, (1, 0, 2)).reshape(own_rows, part_width)
    return mixed, gate_out[None], up_out[None], down_out[None]


def solution(mesh):
    in_specs = (
        P("fs", None),
        P("fs", None),
        P("fs", None),
        P("fs"),
        P(None, "fs", "tp"),
        P(None, "fs", "tp"),
        P(None, "fs", "tp"),
    )
    out_specs = (P("fs", "tp"), P("tp", None, "fs"), P("tp", None, "fs"), P("tp", None, "fs"))
    return jax.shard_map(
        per_device, mesh=mesh, in_specs=in_specs, out_specs=out_specs, check_vma=False
    )
```

```python
import functools

import jax
import jax.numpy as jnp
from jax import lax
from jax.experimental import pallas as pl
from jax.experimental.pallas import tpu as pltpu
from jax.sharding import PartitionSpec as P


HBM = pltpu.MemorySpace.HBM
VMEM = pltpu.MemorySpace.VMEM
SMEM = pltpu.MemorySpace.SMEM


def swap(value, axis, k):
    count = lax.axis_size(axis)
    return lax.ppermute(value, axis, [(i, i ^ k) for i in range(count)])


def partner_orders(count, spread):
    near = [spread] + [k for k in range(1, count // 2) if k != spread]
    far = [k ^ 1 for k in range(count // 2, count)]
    half = len(far) // 2
    order = near[:1] + far[:half] + near[1:] + far[half:]
    first_order = far[:half][::-1] + near[1:] + near[:1] + far[half:]
    return near, far, first_order, order


def make_piece(weight, gain, dest, spread, columns, start, rows):
    spot = (lax.div(dest, spread), start, lax.rem(dest, spread) * columns)
    piece = lax.dynamic_slice(weight, spot, (1, rows, columns))[0]
    if gain is not None:
        piece = piece * gain[start : start + rows, None]
    return piece.astype(jnp.bfloat16)


def act_kernel(count, per_tp, keys, hidden, *refs):
    me_ref, x_ref = refs[:2]
    pieces = refs[2 : 2 + count]
    refs = refs[2 + count :]
    if hidden:
        gate_ref, out_ref, act_ref, held, acc, load_sem, store_sem = refs
    else:
        out_ref, act_ref, held, acc, load_sem, store_sem = refs
    rows = pieces[0].shape[0]
    loads = [
        pltpu.make_async_copy(pieces[j], held.at[j], load_sem.at[j]) for j in range(count)
    ]
    for load in loads:
        load.start()
    stores = []
    for j in range(count):
        slot = me_ref[0] ^ keys[j]
        loads[j].wait()
        store = pltpu.make_async_copy(
            held.at[j], out_ref.at[pl.ds(pl.multiple_of(slot * rows, rows), rows)], store_sem.at[j]
        )
        store.start()
        stores.append(store)
        which = (slot // per_tp ^ me_ref[1]) * per_tp + slot % per_tp
        part = jnp.dot(x_ref[which], held[j], preferred_element_type=jnp.float32)
        if j == 0:
            acc[...] = part
        else:
            acc[...] += part
    if hidden:
        gate = gate_ref[...]
        act_ref[...] = (gate / (1.0 + jnp.exp(-gate)) * acc[...]).astype(jnp.bfloat16)
    else:
        act_ref[...] = acc[...]
    for store in stores:
        store.wait()


def activate(me, x, pieces, keys, per_tp, gate=None):
    count = len(pieces)
    rows, columns = pieces[0].shape
    tokens = x.shape[1]
    args = [me, x, *pieces]
    in_specs = [pl.BlockSpec(memory_space=SMEM), pl.BlockSpec(memory_space=VMEM)]
    in_specs += [pl.BlockSpec(memory_space=HBM)] * count
    if gate is not None:
        args.append(gate)
        in_specs.append(pl.BlockSpec(memory_space=VMEM))
    act_type = jnp.float32 if gate is None else jnp.bfloat16
    return pl.pallas_call(
        functools.partial(act_kernel, count, per_tp, keys, gate is not None),
        in_specs=in_specs,
        out_specs=[pl.BlockSpec(memory_space=HBM), pl.BlockSpec(memory_space=VMEM)],
        out_shape=[
            jax.ShapeDtypeStruct((count * rows, columns), jnp.bfloat16),
            jax.ShapeDtypeStruct((tokens, columns), act_type),
        ],
        scratch_shapes=[
            pltpu.VMEM((count, rows, columns), jnp.bfloat16),
            pltpu.VMEM((tokens, columns), jnp.float32),
            pltpu.SemaphoreType.DMA((count,)),
            pltpu.SemaphoreType.DMA((count,)),
        ],
    )(*args)


def down_kernel(keys, offsets, rows, width, start, aliased, *refs):
    me_ref, hidden_ref, weight_ref = refs[:3]
    count = len(keys)
    pieces = refs[3 : 3 + count]
    refs = refs[3 + count + aliased :]
    out_ref, blocks = refs[0], refs[1:-3]
    held, load_sem, place_sem = refs[-3:]
    loads, places = [], []
    for j in range(count):
        slot = me_ref[0] ^ keys[j]
        spot = held.at[pl.ds(pl.multiple_of(slot * rows, rows), rows)]
        first = pl.multiple_of(slot * width + start, 16)
        piece = pieces[j].at[pl.ds(offsets[j], rows)]
        loads.append(pltpu.make_async_copy(piece, spot, load_sem.at[j]))
        places.append(
            pltpu.make_async_copy(spot, out_ref.at[pl.ds(first, rows)], place_sem.at[j])
        )
    for load in loads:
        load.start()
    for load, place in zip(loads, places):
        load.wait()
        place.start()
    span = held.shape[0] // len(blocks)
    for rel, block_ref in enumerate(blocks):
        block = me_ref[1] ^ rel
        part = lax.dot_general(
            hidden_ref[...],
            held[pl.ds(pl.multiple_of(block * span, span), span)],
            (((1,), (1,)), ((), ())),
            preferred_element_type=jnp.float32,
        )
        block_ref[...] = (part * weight_ref[...]).astype(jnp.bfloat16)
    for place in places:
        place.wait()


def down_partial(me, hidden, weight, pieces, keys, parts, width, start, rows, out):
    count = len(pieces)
    columns = pieces[0].shape[1]
    offsets = [start if piece.shape[0] == width else 0 for piece in pieces]
    tokens = hidden.shape[0]
    block = jax.ShapeDtypeStruct((tokens, count * rows // parts), jnp.bfloat16)
    args = [me, hidden, weight, *pieces]
    in_specs = [pl.BlockSpec(memory_space=SMEM)] + [pl.BlockSpec(memory_space=VMEM)] * 2
    in_specs += [pl.BlockSpec(memory_space=HBM)] * count
    aliases = {}
    if out is not None:
        aliases = {len(args): 0}
        args.append(out)
        in_specs.append(pl.BlockSpec(memory_space=HBM))
    return pl.pallas_call(
        functools.partial(down_kernel, keys, offsets, rows, width, start, len(aliases)),
        in_specs=in_specs,
        out_specs=[pl.BlockSpec(memory_space=HBM)] + [pl.BlockSpec(memory_space=VMEM)] * parts,
        out_shape=[jax.ShapeDtypeStruct((count * width, columns), jnp.bfloat16)] + [block] * parts,
        scratch_shapes=[
            pltpu.VMEM((count * rows, columns), jnp.bfloat16),
            pltpu.SemaphoreType.DMA((count,)),
            pltpu.SemaphoreType.DMA((count,)),
        ],
        input_output_aliases=aliases,
    )(*args)


def in_order(blocks, keys, me):
    stacked = jnp.stack(blocks)
    index = jnp.bitwise_xor(jnp.arange(len(keys)), me)
    where = jnp.argsort(jnp.array(keys))
    return stacked[jnp.take(where, index)]


def make_packet(tokens, routes, route_logits, experts):
    tok_float = tokens.astype(jnp.float32)
    normed = (
        tok_float * lax.rsqrt(jnp.mean(tok_float * tok_float, axis=1, keepdims=True) + 1e-05)
    ).astype(jnp.bfloat16)
    part_width = tokens.shape[1] // lax.axis_size("tp")
    own_cols = lax.dynamic_slice_in_dim(normed, lax.axis_index("tp") * part_width, part_width, 1)
    shares = jax.nn.sigmoid(route_logits - route_logits[:, ::-1])
    expert_ids = lax.broadcasted_iota(jnp.int32, (1, 1, experts), 2)
    weights = jnp.sum(jnp.where(routes[:, :, None] == expert_ids, shares[:, :, None], 0.0), axis=1)
    terms, rest = [], weights
    for _ in range(3):
        term = lax.reduce_precision(rest, 8, 7)
        terms.append(term.astype(jnp.bfloat16))
        rest = rest - term
    extra = jnp.concatenate(terms, axis=1)
    extra = jnp.pad(extra, ((0, 0), (0, -extra.shape[1] % 128)))
    return jnp.concatenate([own_cols, extra], axis=1)


def per_device(tokens, routes, route_logits, norm_gain, gate_weight, up_weight, down_weight):
    experts, width, _ = gate_weight.shape
    fs_count, tp_count = lax.axis_size("fs"), lax.axis_size("tp")
    fs_me, tp_me = lax.axis_index("fs"), lax.axis_index("tp")
    spread = fs_count // experts
    per_tp = fs_count // tp_count
    columns = gate_weight.shape[2] // spread
    own_rows, model = tokens.shape
    part_width = model // tp_count
    me = jnp.stack([fs_me, tp_me]).astype(jnp.int32)
    near, far, first_order, order = partner_orders(fs_count, spread)
    keys = [0] + near + far
    cuts = [0, width // 2, width * 3 // 4, width]
    spans = [(start, end - start) for start, end in zip(cuts, cuts[1:])]

    def fold(weight, gain, k, start=0, rows=width):
        return make_piece(weight, gain, fs_me ^ k, spread, columns, start, rows)

    def send(pieces):
        arrived = {}
        for k, piece in pieces.items():
            arrived[k] = swap(piece, "fs", k)
        return arrived

    first = fold(gate_weight, norm_gain, first_order[0])
    tokens, routes, route_logits, first = lax.optimization_barrier(
        (tokens, routes, route_logits, first)
    )
    packet = make_packet(tokens, routes, route_logits, experts)
    packet, gate_weight, first = lax.optimization_barrier((packet, gate_weight, first))
    groups = list(range(spread, fs_count, spread))
    held = [packet] + [swap(packet, "fs", k) for k in groups]
    gate_folds = {k: fold(gate_weight, norm_gain, k) for k in first_order[1:]}
    gate_folds, up_weight = lax.optimization_barrier((gate_folds, up_weight))
    gate_sent = send({first_order[0]: first, **gate_folds})
    up_folds = {k: fold(up_weight, norm_gain, k) for k in order}
    up_folds, down_weight = lax.optimization_barrier((up_folds, down_weight))
    up_sent = send(up_folds)
    down_folds = {k: fold(down_weight, None, k) for k in near}
    down_near = send(down_folds)
    down_far = [{k: fold(down_weight, None, k, *span) for k in far} for span in spans]
    down_sent = [send(folds) for folds in down_far]
    down_far, gate_weight, up_weight, down_weight = lax.optimization_barrier(
        (down_far, gate_weight, up_weight, down_weight)
    )
    gate_pieces = [fold(gate_weight, norm_gain, 0)] + [gate_sent[k] for k in keys[1:]]
    up_pieces = [fold(up_weight, norm_gain, 0)] + [up_sent[k] for k in keys[1:]]
    down_pieces = [
        [fold(down_weight, None, 0)] + [{**down_near, **sent}[k] for k in keys[1:]]
        for sent in down_sent
    ]

    held = in_order(held, list(range(experts)), lax.div(fs_me, spread))
    held = [held] + [swap(held, "fs", k) for k in range(1, spread)]
    held = in_order(held, list(range(spread)), lax.rem(fs_me, spread))
    gathered = jnp.swapaxes(held, 0, 1).reshape(fs_count * own_rows, packet.shape[1])
    block = gathered[:, :part_width]
    term_cols = gathered[:, part_width : part_width + 3 * experts].astype(jnp.float32)
    row_weights = jnp.sum(term_cols.reshape(-1, 3, experts), axis=1)
    mine = lax.broadcasted_iota(jnp.int32, (1, experts), 1) == lax.div(fs_me, spread)
    row_weight = jnp.sum(jnp.where(mine, row_weights, 0.0), axis=1, keepdims=True)
    blocks = jnp.stack([block] + [swap(block, "tp", k) for k in range(1, tp_count)])
    x = blocks.reshape(tp_count, -1, per_tp, width)
    x = jnp.transpose(x, (0, 2, 1, 3)).reshape(fs_count, -1, width)

    gate_out, gate_act = activate(me, x, gate_pieces, keys, per_tp)
    up_out, hidden = activate(me, x, up_pieces, keys, per_tp, gate_act)

    down_out = None
    totals = []
    for span, pieces in zip(spans, down_pieces):
        down_out, *parts = down_partial(
            me, hidden, row_weight, pieces, keys, tp_count, width, *span, down_out
        )
        total = parts[0].astype(jnp.float32)
        for k in range(1, tp_count):
            total = total + swap(parts[k], "tp", k).astype(jnp.float32)
        totals.append(total.astype(jnp.bfloat16).reshape(fs_count, own_rows, -1))
    done = []
    for group in [totals[:-1], totals[-1:]]:
        away = jnp.concatenate(group, axis=2)
        back = lax.all_to_all(away, "fs", split_axis=0, concat_axis=0, tiled=True)
        ends = [part.shape[2] for part in group]
        ends = [sum(ends[: i + 1]) for i in range(len(ends) - 1)]
        back = jnp.sum(back.astype(jnp.float32), axis=0).astype(jnp.bfloat16)
        done += jnp.split(back, ends, axis=1)
    mixed = jnp.concatenate([part.reshape(own_rows, per_tp, -1) for part in done], axis=2)
    return mixed.reshape(own_rows, part_width), gate_out[None], up_out[None], down_out[None]


def solution(mesh):
    in_specs = (
        P("fs", None),
        P("fs", None),
        P("fs", None),
        P("fs"),
        P(None, "fs", "tp"),
        P(None, "fs", "tp"),
        P(None, "fs", "tp"),
    )
    out_specs = (P("fs", "tp"), P("tp", None, "fs"), P("tp", None, "fs"), P("tp", None, "fs"))

    return jax.shard_map(
        per_device, mesh=mesh, in_specs=in_specs, out_specs=out_specs, check_vma=False
    )
```

```python
import functools

import jax
import jax.numpy as jnp
from jax import lax
from jax.experimental import pallas as pl
from jax.experimental.pallas import tpu as pltpu
from jax.sharding import PartitionSpec as P


CAP = 30

HBM = pltpu.MemorySpace.HBM
VMEM = pltpu.MemorySpace.VMEM
SMEM = pltpu.MemorySpace.SMEM


def swap(value, axis, k):
    count = lax.axis_size(axis)
    return lax.ppermute(value, axis, [(i, i ^ k) for i in range(count)])


def partner_orders(count, spread):
    near = [spread] + [k for k in range(1, count // 2) if k != spread]
    far = [k ^ 1 for k in range(count // 2, count)]
    half = len(far) // 2
    order = near[:1] + far[:half] + near[1:] + far[half:]
    first_order = far[:half][::-1] + near[1:] + near[:1] + far[half:]
    return near, far, first_order, order


def make_piece(weight, gain, dest, spread, columns, start, rows):
    spot = (lax.div(dest, spread), start, lax.rem(dest, spread) * columns)
    piece = lax.dynamic_slice(weight, spot, (1, rows, columns))[0]
    if gain is not None:
        piece = piece * gain[start : start + rows, None]
    return piece.astype(jnp.bfloat16)


def act_kernel(count, per_tp, keys, hidden, *refs):
    me_ref, x_ref = refs[:2]
    pieces = refs[2 : 2 + count]
    refs = refs[2 + count :]
    if hidden:
        gate_ref, out_ref, act_ref, held, acc, load_sem, store_sem = refs
    else:
        out_ref, act_ref, held, acc, load_sem, store_sem = refs
    rows = pieces[0].shape[0]
    loads = [
        pltpu.make_async_copy(pieces[j], held.at[j], load_sem.at[j]) for j in range(count)
    ]
    for load in loads:
        load.start()
    stores = []
    for j in range(count):
        slot = me_ref[0] ^ keys[j]
        loads[j].wait()
        store = pltpu.make_async_copy(
            held.at[j], out_ref.at[pl.ds(pl.multiple_of(slot * rows, rows), rows)], store_sem.at[j]
        )
        store.start()
        stores.append(store)
        which = (slot // per_tp ^ me_ref[1]) * per_tp + slot % per_tp
        part = jnp.dot(x_ref[which], held[j], preferred_element_type=jnp.float32)
        if j == 0:
            acc[...] = part
        else:
            acc[...] += part
    if hidden:
        gate = gate_ref[...]
        act_ref[...] = (gate / (1.0 + jnp.exp(-gate)) * acc[...]).astype(jnp.bfloat16)
    else:
        act_ref[...] = acc[...]
    for store in stores:
        store.wait()


def activate(me, x, pieces, keys, per_tp, gate=None):
    count = len(pieces)
    rows, columns = pieces[0].shape
    tokens = x.shape[1]
    args = [me, x, *pieces]
    in_specs = [pl.BlockSpec(memory_space=SMEM), pl.BlockSpec(memory_space=VMEM)]
    in_specs += [pl.BlockSpec(memory_space=HBM)] * count
    if gate is not None:
        args.append(gate)
        in_specs.append(pl.BlockSpec(memory_space=VMEM))
    act_type = jnp.float32 if gate is None else jnp.bfloat16
    return pl.pallas_call(
        functools.partial(act_kernel, count, per_tp, keys, gate is not None),
        in_specs=in_specs,
        out_specs=[pl.BlockSpec(memory_space=HBM), pl.BlockSpec(memory_space=VMEM)],
        out_shape=[
            jax.ShapeDtypeStruct((count * rows, columns), jnp.bfloat16),
            jax.ShapeDtypeStruct((tokens, columns), act_type),
        ],
        scratch_shapes=[
            pltpu.VMEM((count, rows, columns), jnp.bfloat16),
            pltpu.VMEM((tokens, columns), jnp.float32),
            pltpu.SemaphoreType.DMA((count,)),
            pltpu.SemaphoreType.DMA((count,)),
        ],
    )(*args)


def fetch(keys, offsets, rows, width, start, me_ref, pieces, out_ref, held, load_sem, place_sem):
    loads, places = [], []
    for j in range(len(keys)):
        slot = me_ref[0] ^ keys[j]
        spot = held.at[pl.ds(pl.multiple_of(slot * rows, rows), rows)]
        piece = pieces[j].at[pl.ds(offsets[j], rows)]
        loads.append(pltpu.make_async_copy(piece, spot, load_sem.at[j]))
        if out_ref is not None:
            first = pl.multiple_of(slot * width + start, 16)
            places.append(
                pltpu.make_async_copy(spot, out_ref.at[pl.ds(first, rows)], place_sem.at[j])
            )
    return loads, places


def down_kernel(keys, offsets, rows, me_ref, hidden_ref, *refs):
    pieces, blocks = refs[: len(keys)], refs[len(keys) : -6]
    hidden, held, sums, hidden_sem, load_sem, store_sem = refs[-6:]
    loads, _ = fetch(keys, offsets, rows, 0, 0, me_ref, pieces, None, held, load_sem, None)
    loads.append(pltpu.make_async_copy(hidden_ref, hidden, hidden_sem))
    for load in loads:
        load.start()
    for load in loads:
        load.wait()
    span = held.shape[0] // len(blocks)
    stores = []
    for rel in reversed(range(len(blocks))):
        block = me_ref[1] ^ rel
        part = lax.dot_general(
            hidden[...],
            held[pl.ds(pl.multiple_of(block * span, span), span)],
            (((1,), (1,)), ((), ())),
            preferred_element_type=jnp.float32,
        )
        sums[rel] = part.astype(jnp.bfloat16)
        store = pltpu.make_async_copy(sums.at[rel], blocks[rel], store_sem.at[rel])
        store.start()
        stores.append(store)
    for store in stores:
        store.wait()


def down_partial(me, hidden, pieces, keys, parts, width, start, rows):
    count = len(pieces)
    columns = pieces[0].shape[1]
    offsets = [start if piece.shape[0] == width else 0 for piece in pieces]
    block = jax.ShapeDtypeStruct((hidden.shape[0], count * rows // parts), jnp.bfloat16)
    return pl.pallas_call(
        functools.partial(down_kernel, keys, offsets, rows),
        in_specs=[pl.BlockSpec(memory_space=SMEM)]
        + [pl.BlockSpec(memory_space=HBM)] * (1 + count),
        out_specs=[pl.BlockSpec(memory_space=HBM)] * parts,
        out_shape=[block] * parts,
        scratch_shapes=[
            pltpu.VMEM(hidden.shape, jnp.bfloat16),
            pltpu.VMEM((count * rows, columns), jnp.bfloat16),
            pltpu.VMEM((parts,) + block.shape, jnp.bfloat16),
            pltpu.SemaphoreType.DMA,
            pltpu.SemaphoreType.DMA((count,)),
            pltpu.SemaphoreType.DMA((parts,)),
        ],
    )(me, hidden, *pieces)


def place_kernel(keys, offsets, rows, width, start, aliased, me_ref, *refs):
    pieces = refs[: len(keys)]
    out_ref, held, load_sem, place_sem = refs[len(keys) + aliased :]
    loads, places = fetch(
        keys, offsets, rows, width, start, me_ref, pieces, out_ref, held, load_sem, place_sem
    )
    for load in loads:
        load.start()
    for load, place in zip(loads, places):
        load.wait()
        place.start()
    for place in places:
        place.wait()


def place_chunk(me, pieces, keys, width, start, rows, out):
    count = len(pieces)
    columns = pieces[0].shape[1]
    offsets = [start if piece.shape[0] == width else 0 for piece in pieces]
    args = [me, *pieces]
    aliases = {}
    if out is not None:
        aliases = {len(args): 0}
        args.append(out)
    return pl.pallas_call(
        functools.partial(place_kernel, keys, offsets, rows, width, start, len(aliases)),
        in_specs=[pl.BlockSpec(memory_space=SMEM)]
        + [pl.BlockSpec(memory_space=HBM)] * (len(args) - 1),
        out_specs=pl.BlockSpec(memory_space=HBM),
        out_shape=jax.ShapeDtypeStruct((count * width, columns), jnp.bfloat16),
        scratch_shapes=[
            pltpu.VMEM((count * rows, columns), jnp.bfloat16),
            pltpu.SemaphoreType.DMA((count,)),
            pltpu.SemaphoreType.DMA((count,)),
        ],
        input_output_aliases=aliases,
    )(*args)


def in_order(blocks, keys, me):
    stacked = jnp.stack(blocks)
    index = jnp.bitwise_xor(jnp.arange(len(keys)), me)
    where = jnp.argsort(jnp.array(keys))
    return stacked[jnp.take(where, index)]


def pack_rows(tokens, routes, route_logits, experts):
    tok_float = tokens.astype(jnp.float32)
    normed = (
        tok_float * lax.rsqrt(jnp.mean(tok_float * tok_float, axis=1, keepdims=True) + 1e-05)
    ).astype(jnp.bfloat16)
    part_width = tokens.shape[1] // lax.axis_size("tp")
    own_cols = lax.dynamic_slice_in_dim(normed, lax.axis_index("tp") * part_width, part_width, 1)
    shares = jax.nn.sigmoid(route_logits - route_logits[:, ::-1])
    expert_ids = lax.broadcasted_iota(jnp.int32, (1, 1, experts), 2)
    picks = routes[:, :, None] == expert_ids
    member = jnp.sum(picks.astype(jnp.int32), axis=1)
    rows = lax.broadcasted_iota(jnp.int32, (1, tokens.shape[0]), 1)
    earlier = jnp.transpose(rows) > rows
    position = jnp.sum(jnp.where(earlier[:, :, None], member[None], 0), axis=1)
    slots = -(-CAP // 16) * 16
    slot_ids = lax.broadcasted_iota(jnp.int32, (1, 1, slots), 2)
    placing = (position[:, :, None] == slot_ids) & (member[:, :, None] > 0)
    packed = jnp.einsum(
        "rec,rd->ecd", placing.astype(jnp.bfloat16), own_cols, preferred_element_type=jnp.float32
    ).astype(jnp.bfloat16)
    weights = jnp.sum(jnp.where(picks, shares[:, :, None], 0.0), axis=1)
    return packed, jnp.where(placing, weights[:, :, None], 0.0)


def per_device(tokens, routes, route_logits, norm_gain, gate_weight, up_weight, down_weight):
    experts, width, _ = gate_weight.shape
    fs_count, tp_count = lax.axis_size("fs"), lax.axis_size("tp")
    fs_me, tp_me = lax.axis_index("fs"), lax.axis_index("tp")
    spread = fs_count // experts
    per_tp = fs_count // tp_count
    columns = gate_weight.shape[2] // spread
    own_rows, model = tokens.shape
    part_width = model // tp_count
    me = jnp.stack([fs_me, tp_me]).astype(jnp.int32)
    near, far, first_order, order = partner_orders(fs_count, spread)
    keys = [0] + near + far
    cuts = [0, width // 2, width * 3 // 4, width * 7 // 8, width]
    spans = [(start, end - start) for start, end in zip(cuts, cuts[1:])]

    def fold(weight, gain, k, start=0, rows=width):
        return make_piece(weight, gain, fs_me ^ k, spread, columns, start, rows)

    def send(pieces):
        arrived = {}
        for k, piece in pieces.items():
            arrived[k] = swap(piece, "fs", k)
        return arrived

    first = fold(gate_weight, norm_gain, first_order[0])
    tokens, routes, route_logits, first = lax.optimization_barrier(
        (tokens, routes, route_logits, first)
    )
    packed, combine = pack_rows(tokens, routes, route_logits, experts)
    packed, gate_weight, first = lax.optimization_barrier((packed, gate_weight, first))
    plane = lax.div(fs_me, spread)
    packets = [lax.dynamic_index_in_dim(packed, plane ^ e, 0, False) for e in range(experts)]
    held = packets[:1] + [swap(packets[e], "fs", e * spread) for e in range(1, experts)]
    gate_folds = {k: fold(gate_weight, norm_gain, k) for k in first_order[1:]}
    gate_folds, up_weight = lax.optimization_barrier((gate_folds, up_weight))
    gate_sent = send({first_order[0]: first, **gate_folds})
    up_folds = {k: fold(up_weight, norm_gain, k) for k in order}
    up_folds, down_weight = lax.optimization_barrier((up_folds, down_weight))
    up_sent = send(up_folds)
    down_folds = {k: fold(down_weight, None, k) for k in near}
    down_near = send(down_folds)
    down_far = [{k: fold(down_weight, None, k, *span) for k in far} for span in spans]
    down_sent = [send(folds) for folds in down_far]
    down_far, gate_weight, up_weight, down_weight = lax.optimization_barrier(
        (down_far, gate_weight, up_weight, down_weight)
    )
    gate_pieces = [fold(gate_weight, norm_gain, 0)] + [gate_sent[k] for k in keys[1:]]
    up_pieces = [fold(up_weight, norm_gain, 0)] + [up_sent[k] for k in keys[1:]]
    down_pieces = [
        [fold(down_weight, None, 0)] + [{**down_near, **sent}[k] for k in keys[1:]]
        for sent in down_sent
    ]

    held = in_order(held, list(range(experts)), plane)
    held = [held] + [swap(held, "fs", k) for k in range(1, spread)]
    held = in_order(held, list(range(spread)), lax.rem(fs_me, spread))
    block = jnp.swapaxes(held, 0, 1).reshape(-1, part_width)
    blocks = jnp.stack([block] + [swap(block, "tp", k) for k in range(1, tp_count)])
    x = blocks.reshape(tp_count, -1, per_tp, width)
    x = jnp.transpose(x, (0, 2, 1, 3)).reshape(fs_count, -1, width)

    gate_out, gate_act = activate(me, x, gate_pieces, keys, per_tp)
    up_out, hidden = activate(me, x, up_pieces, keys, per_tp, gate_act)

    down_out = None
    totals = []
    for span, pieces in zip(spans, down_pieces):
        parts = down_partial(me, hidden, pieces, keys, tp_count, width, *span)
        down_out = place_chunk(me, pieces, keys, width, *span, down_out)
        total = parts[0].astype(jnp.float32)
        for k in range(1, tp_count):
            total = total + swap(parts[k], "tp", k).astype(jnp.float32)
        totals.append(total.astype(jnp.bfloat16).reshape(fs_count, -1, total.shape[1]))
    combine = jnp.broadcast_to(
        combine[:, :, None], (own_rows, experts, spread, combine.shape[2])
    ).reshape(own_rows, -1)
    done = []
    for group in [totals[:2], totals[2:]]:
        away = jnp.concatenate(group, axis=2)
        back = lax.all_to_all(away, "fs", split_axis=0, concat_axis=0, tiled=True)
        ends = [part.shape[2] for part in group]
        ends = [sum(ends[: i + 1]) for i in range(len(ends) - 1)]
        back = back.reshape(-1, back.shape[2]).astype(jnp.float32)
        back = jnp.dot(combine, back, precision=lax.Precision.HIGHEST).astype(jnp.bfloat16)
        done += jnp.split(back, ends, axis=1)
    mixed = jnp.concatenate([part.reshape(own_rows, per_tp, -1) for part in done], axis=2)
    return mixed.reshape(own_rows, part_width), gate_out[None], up_out[None], down_out[None]


def solution(mesh):
    in_specs = (
        P("fs", None),
        P("fs", None),
        P("fs", None),
        P("fs"),
        P(None, "fs", "tp"),
        P(None, "fs", "tp"),
        P(None, "fs", "tp"),
    )
    out_specs = (P("fs", "tp"), P("tp", None, "fs"), P("tp", None, "fs"), P("tp", None, "fs"))

    return jax.shard_map(
        per_device, mesh=mesh, in_specs=in_specs, out_specs=out_specs, check_vma=False
    )
```

```python
import functools

import jax
import jax.numpy as jnp
from jax import lax
from jax.experimental import pallas as pl
from jax.experimental.pallas import tpu as pltpu
from jax.sharding import PartitionSpec as P


CAP = 30

HBM = pltpu.MemorySpace.HBM
VMEM = pltpu.MemorySpace.VMEM


def swap(value, axis, k):
    count = lax.axis_size(axis)
    return lax.ppermute(value, axis, [(i, i ^ k) for i in range(count)])


def partner_orders(count, spread):
    near = [spread] + [k for k in range(1, count // 2) if k != spread]
    far = [k ^ 1 for k in range(count // 2, count)]
    half = len(far) // 2
    order = near[:1] + far[:half] + near[1:] + far[half:]
    first_order = far[:half][::-1] + near[1:] + near[:1] + far[half:]
    return near, far, first_order, order


def make_piece(weight, gain, dest, spread, columns, start, rows):
    spot = (lax.div(dest, spread), start, lax.rem(dest, spread) * columns)
    piece = lax.dynamic_slice(weight, spot, (1, rows, columns))[0]
    if gain is not None:
        piece = piece * gain[start : start + rows, None]
    return piece.astype(jnp.bfloat16)


def act_kernel(count, per_tp, keys, hidden, *refs):
    x_ref, pieces, refs = refs[0], refs[1 : 1 + count], refs[1 + count :]
    if hidden:
        gate_ref, out_ref, act_ref, held, acc, load_sem, store_sem = refs
    else:
        out_ref, act_ref, held, acc, load_sem, store_sem = refs
    rows = pieces[0].shape[0]
    loads = [
        pltpu.make_async_copy(pieces[j], held.at[j], load_sem.at[j]) for j in range(count)
    ]
    for load in loads:
        load.start()
    stores = []
    for j in range(count):
        slot = lax.axis_index("fs") ^ keys[j]
        loads[j].wait()
        store = pltpu.make_async_copy(
            held.at[j], out_ref.at[pl.ds(pl.multiple_of(slot * rows, rows), rows)], store_sem.at[j]
        )
        store.start()
        stores.append(store)
        which = (slot // per_tp ^ lax.axis_index("tp")) * per_tp + slot % per_tp
        part = jnp.dot(x_ref[which], held[j], preferred_element_type=jnp.float32)
        if j == 0:
            acc[...] = part
        else:
            acc[...] += part
    if hidden:
        gate = gate_ref[...]
        act_ref[...] = (gate / (1.0 + jnp.exp(-gate)) * acc[...]).astype(jnp.bfloat16)
    else:
        act_ref[...] = acc[...]
    for store in stores:
        store.wait()


def activate(x, pieces, keys, per_tp, gate=None):
    count = len(pieces)
    rows, columns = pieces[0].shape
    tokens = x.shape[1]
    args = [x, *pieces]
    in_specs = [pl.BlockSpec(memory_space=VMEM)]
    in_specs += [pl.BlockSpec(memory_space=HBM)] * count
    if gate is not None:
        args.append(gate)
        in_specs.append(pl.BlockSpec(memory_space=VMEM))
    act_type = jnp.float32 if gate is None else jnp.bfloat16
    return pl.pallas_call(
        functools.partial(act_kernel, count, per_tp, keys, gate is not None),
        in_specs=in_specs,
        out_specs=[pl.BlockSpec(memory_space=HBM), pl.BlockSpec(memory_space=VMEM)],
        out_shape=[
            jax.ShapeDtypeStruct((count * rows, columns), jnp.bfloat16),
            jax.ShapeDtypeStruct((tokens, columns), act_type),
        ],
        scratch_shapes=[
            pltpu.VMEM((count, rows, columns), jnp.bfloat16),
            pltpu.VMEM((tokens, columns), jnp.float32),
            pltpu.SemaphoreType.DMA((count,)),
            pltpu.SemaphoreType.DMA((count,)),
        ],
    )(*args)


def down_kernel(keys, offsets, rows, hidden_ref, *refs):
    pieces, blocks = refs[: len(keys)], refs[len(keys) : -6]
    hidden, held, sums, hidden_sem, load_sem, store_sem = refs[-6:]
    loads = []
    for j, key in enumerate(keys):
        spot = held.at[pl.ds(pl.multiple_of((lax.axis_index("fs") ^ key) * rows, rows), rows)]
        piece = pieces[j].at[pl.ds(offsets[j], rows)]
        loads.append(pltpu.make_async_copy(piece, spot, load_sem.at[j]))
    loads.append(pltpu.make_async_copy(hidden_ref, hidden, hidden_sem))
    for load in loads:
        load.start()
    for load in loads:
        load.wait()
    span = held.shape[0] // len(blocks)
    stores = []
    for rel in reversed(range(len(blocks))):
        block = lax.axis_index("tp") ^ rel
        part = lax.dot_general(
            hidden[...],
            held[pl.ds(pl.multiple_of(block * span, span), span)],
            (((1,), (1,)), ((), ())),
            preferred_element_type=jnp.float32,
        )
        sums[rel] = part.astype(jnp.bfloat16)
        store = pltpu.make_async_copy(sums.at[rel], blocks[rel], store_sem.at[rel])
        store.start()
        stores.append(store)
    for store in stores:
        store.wait()


def down_partial(hidden, pieces, keys, parts, width, start, rows):
    count = len(pieces)
    columns = pieces[0].shape[1]
    offsets = [start if piece.shape[0] == width else 0 for piece in pieces]
    block = jax.ShapeDtypeStruct((hidden.shape[0], count * rows // parts), jnp.bfloat16)
    return pl.pallas_call(
        functools.partial(down_kernel, keys, offsets, rows),
        in_specs=[pl.BlockSpec(memory_space=HBM)] * (1 + count),
        out_specs=[pl.BlockSpec(memory_space=HBM)] * parts,
        out_shape=[block] * parts,
        scratch_shapes=[
            pltpu.VMEM(hidden.shape, jnp.bfloat16),
            pltpu.VMEM((count * rows, columns), jnp.bfloat16),
            pltpu.VMEM((parts,) + block.shape, jnp.bfloat16),
            pltpu.SemaphoreType.DMA,
            pltpu.SemaphoreType.DMA((count,)),
            pltpu.SemaphoreType.DMA((parts,)),
        ],
    )(hidden, *pieces)


def place_kernel(moves, width, aliased, *refs):
    pieces = refs[: len(moves)]
    out_ref, held, load_sem, place_sem = refs[len(moves) + aliased :]
    loads, places = [], []
    place = 0
    for j, (key, offset, start, rows) in enumerate(moves):
        spot = held.at[pl.ds(place, rows)]
        first = pl.multiple_of((lax.axis_index("fs") ^ key) * width + start, 16)
        piece = pieces[j].at[pl.ds(offset, rows)]
        loads.append(pltpu.make_async_copy(piece, spot, load_sem.at[j]))
        places.append(pltpu.make_async_copy(spot, out_ref.at[pl.ds(first, rows)], place_sem.at[j]))
        place += rows
    for load in loads:
        load.start()
    for load, place in zip(loads, places):
        load.wait()
        place.start()
    for place in places:
        place.wait()


def place_chunks(chunks, keys, width, spans, out):
    args, moves = [], []
    for pieces, (start, rows) in zip(chunks, spans):
        for key, piece in zip(keys, pieces):
            args.append(piece)
            moves.append((key, start if piece.shape[0] == width else 0, start, rows))
    columns = args[0].shape[1]
    aliases = {}
    if out is not None:
        aliases = {len(args): 0}
        args.append(out)
    return pl.pallas_call(
        functools.partial(place_kernel, moves, width, len(aliases)),
        in_specs=[pl.BlockSpec(memory_space=HBM)] * len(args),
        out_specs=pl.BlockSpec(memory_space=HBM),
        out_shape=jax.ShapeDtypeStruct((len(keys) * width, columns), jnp.bfloat16),
        scratch_shapes=[
            pltpu.VMEM((len(keys) * sum(rows for _, rows in spans), columns), jnp.bfloat16),
            pltpu.SemaphoreType.DMA((len(moves),)),
            pltpu.SemaphoreType.DMA((len(moves),)),
        ],
        input_output_aliases=aliases,
    )(*args)


def in_order(blocks, keys, me):
    stacked = jnp.stack(blocks)
    index = jnp.bitwise_xor(jnp.arange(len(keys)), me)
    where = jnp.argsort(jnp.array(keys))
    return stacked[jnp.take(where, index)]


def pack_rows(tokens, routes, route_logits, experts):
    tok_float = tokens.astype(jnp.float32)
    normed = (
        tok_float * lax.rsqrt(jnp.mean(tok_float * tok_float, axis=1, keepdims=True) + 1e-05)
    ).astype(jnp.bfloat16)
    part_width = tokens.shape[1] // lax.axis_size("tp")
    own_cols = lax.dynamic_slice_in_dim(normed, lax.axis_index("tp") * part_width, part_width, 1)
    shares = jax.nn.sigmoid(route_logits - route_logits[:, ::-1])
    expert_ids = lax.broadcasted_iota(jnp.int32, (1, 1, experts), 2)
    picks = routes[:, :, None] == expert_ids
    member = jnp.sum(picks.astype(jnp.int32), axis=1)
    rows = lax.broadcasted_iota(jnp.int32, (1, tokens.shape[0]), 1)
    earlier = jnp.transpose(rows) > rows
    position = jnp.sum(jnp.where(earlier[:, :, None], member[None], 0), axis=1)
    slots = -(-CAP // 16) * 16
    slot_ids = lax.broadcasted_iota(jnp.int32, (1, 1, slots), 2)
    placing = (position[:, :, None] == slot_ids) & (member[:, :, None] > 0)
    packed = jnp.einsum(
        "rec,rd->ecd", placing.astype(jnp.bfloat16), own_cols, preferred_element_type=jnp.float32
    ).astype(jnp.bfloat16)
    weights = jnp.sum(jnp.where(picks, shares[:, :, None], 0.0), axis=1)
    return packed, jnp.where(placing, weights[:, :, None], 0.0)


def per_device(tokens, routes, route_logits, norm_gain, gate_weight, up_weight, down_weight):
    experts, width, _ = gate_weight.shape
    fs_count, tp_count = lax.axis_size("fs"), lax.axis_size("tp")
    fs_me = lax.axis_index("fs")
    spread = fs_count // experts
    per_tp = fs_count // tp_count
    columns = gate_weight.shape[2] // spread
    own_rows, model = tokens.shape
    part_width = model // tp_count
    near, far, first_order, order = partner_orders(fs_count, spread)
    keys = [0] + near + far
    cuts = [0, width // 2, width * 3 // 4, width * 7 // 8, width]
    spans = [(start, end - start) for start, end in zip(cuts, cuts[1:])]

    def fold(weight, gain, k, start=0, rows=width):
        return make_piece(weight, gain, fs_me ^ k, spread, columns, start, rows)

    def send(pieces):
        arrived = {}
        for k, piece in pieces.items():
            arrived[k] = swap(piece, "fs", k)
        return arrived

    first = fold(gate_weight, norm_gain, first_order[0])
    tokens, routes, route_logits, first = lax.optimization_barrier(
        (tokens, routes, route_logits, first)
    )
    packed, combine = pack_rows(tokens, routes, route_logits, experts)
    packed, gate_weight, first = lax.optimization_barrier((packed, gate_weight, first))
    plane = lax.div(fs_me, spread)
    packets = [lax.dynamic_index_in_dim(packed, plane ^ e, 0, False) for e in range(experts)]
    held = packets[:1] + [swap(packets[e], "fs", e * spread) for e in range(1, experts)]
    gate_folds = {k: fold(gate_weight, norm_gain, k) for k in first_order[1:]}
    gate_folds, up_weight = lax.optimization_barrier((gate_folds, up_weight))
    gate_sent = send({first_order[0]: first, **gate_folds})
    up_folds = {k: fold(up_weight, norm_gain, k) for k in order}
    up_folds, down_weight = lax.optimization_barrier((up_folds, down_weight))
    up_sent = send(up_folds)
    down_folds = {k: fold(down_weight, None, k) for k in near}
    down_near = send(down_folds)
    down_far = [{k: fold(down_weight, None, k, *span) for k in far} for span in spans]
    down_sent = [send(folds) for folds in down_far]
    down_far, gate_weight, up_weight, down_weight = lax.optimization_barrier(
        (down_far, gate_weight, up_weight, down_weight)
    )
    gate_pieces = [fold(gate_weight, norm_gain, 0)] + [gate_sent[k] for k in keys[1:]]
    up_pieces = [fold(up_weight, norm_gain, 0)] + [up_sent[k] for k in keys[1:]]
    down_pieces = [
        [fold(down_weight, None, 0)] + [{**down_near, **sent}[k] for k in keys[1:]]
        for sent in down_sent
    ]

    held = in_order(held, list(range(experts)), plane)
    held = [held] + [swap(held, "fs", k) for k in range(1, spread)]
    held = in_order(held, list(range(spread)), lax.rem(fs_me, spread))
    block = jnp.swapaxes(held, 0, 1).reshape(-1, part_width)
    blocks = jnp.stack([block] + [swap(block, "tp", k) for k in range(1, tp_count)])
    x = blocks.reshape(tp_count, -1, per_tp, width)
    x = jnp.transpose(x, (0, 2, 1, 3)).reshape(fs_count, -1, width)

    gate_out, gate_act = activate(x, gate_pieces, keys, per_tp)
    up_out, hidden = activate(x, up_pieces, keys, per_tp, gate_act)

    down_out = None
    totals = []
    for c, (span, pieces) in enumerate(zip(spans, down_pieces)):
        parts = down_partial(hidden, pieces, keys, tp_count, width, *span)
        if c < 2 or c == len(spans) - 1:
            first = min(c, 2)
            down_out = place_chunks(
                down_pieces[first : c + 1], keys, width, spans[first : c + 1], down_out
            )
        total = parts[0].astype(jnp.float32)
        for k in reversed(range(1, tp_count)):
            total = total + swap(parts[k], "tp", k).astype(jnp.float32)
        totals.append(total.astype(jnp.bfloat16).reshape(fs_count, -1, total.shape[1]))
    combine = jnp.broadcast_to(
        combine[:, :, None], (own_rows, experts, spread, combine.shape[2])
    ).reshape(own_rows, -1)
    done = []
    for group in [totals[:2], totals[2:]]:
        away = jnp.concatenate(group, axis=2)
        back = lax.all_to_all(away, "fs", split_axis=0, concat_axis=0, tiled=True)
        ends = [part.shape[2] for part in group]
        ends = [sum(ends[: i + 1]) for i in range(len(ends) - 1)]
        back = back.reshape(-1, back.shape[2]).astype(jnp.float32)
        back = jnp.dot(combine, back, precision=lax.Precision.HIGHEST).astype(jnp.bfloat16)
        done += jnp.split(back, ends, axis=1)
    mixed = jnp.concatenate([part.reshape(own_rows, per_tp, -1) for part in done], axis=2)
    return mixed.reshape(own_rows, part_width), gate_out[None], up_out[None], down_out[None]


def solution(mesh):
    in_specs = (
        P("fs", None),
        P("fs", None),
        P("fs", None),
        P("fs"),
        P(None, "fs", "tp"),
        P(None, "fs", "tp"),
        P(None, "fs", "tp"),
    )
    out_specs = (P("fs", "tp"), P("tp", None, "fs"), P("tp", None, "fs"), P("tp", None, "fs"))

    return jax.shard_map(
        per_device, mesh=mesh, in_specs=in_specs, out_specs=out_specs, check_vma=False
    )
```
